32 devices in a mesh: sp: 8 (over z, y), dp: 4 (over x, core).
Axes of the slice: x: 2, y: 2, z: 4, core: 2. Of those that a mesh axis runs over, the one named last changes fastest.
Arguments:
- residual_input: bfloat16 [4, 1024, 2048], P('dp', 'sp'), may hold values from -6 to 6
- queries: bfloat16 [4, 1024, 512], P('dp', 'sp'), may hold values from -6 to 6
- keys: bfloat16 [4, 1024, 512], P('dp', 'sp'), may hold values from -6 to 6
- values: bfloat16 [4, 1024, 1024], P('dp', 'sp'), may hold values from -6 to 6
- gate_logits: bfloat16 [4, 1024, 32], P('dp', 'sp'), may hold values from -6 to 6
- retention_offset: float32 [8, 2], P('sp'), may hold values from 3 to 12
- log_forget_extra: float32 [4, 8, 1024], P('dp', 'sp'), may hold values from -2.76 to 0
- lane_amplifier: float32 [1024], P('sp'), may hold values from 0.1 to 1.9
- output_gate_logits: bfloat16 [4, 1024, 1024], P('dp', 'sp'), may hold values from -6 to 6
- output_projection: bfloat16 [1024, 2048], P(None, 'dp'), may hold values from -0.1875 to 0.1875
- cell_norm_gain: float32 [2048], replicated, may hold values from 0.1 to 1.9
- expert_norm_gain: float32 [2048], replicated, may hold values from 0.1 to 1.9
- expert_index: int32 [4, 1024, 2], P('dp', 'sp'), may hold values from 0 to 31, all different within a row; in each aligned block of 128 rows (0 to 127, 128 to 255, ..., all dimensions but the last counted through in order) at most 16 rows name the same one
- group_mixing_weight: float32 [4, 1024, 4], P('dp', 'sp'), may hold values from 0.05 to 1
- within_group_weight: float32 [4, 1024, 2], P('dp', 'sp'), may hold values from 0.1 to 1
- gate_weight: bfloat16 [32, 2048, 1024], P(('sp', 'dp')), may hold values from -0.125 to 0.125
- up_weight: bfloat16 [32, 2048, 1024], P(('sp', 'dp')), may hold values from -0.125 to 0.125
- down_weight: bfloat16 [32, 1024, 2048], P(('sp', 'dp')), may hold values from -0.75 to 0.75
Outputs:
- stream_out: bfloat16 [4, 1024, 2048], P('dp', 'sp')
The draws below stay inside these ranges and needn't reach their ends.
Inputs may be any that keep to these rules, and one draw needn't show every extreme that they name: `expert_index`: A token's two experts differ; among the 128 tokens of one device no expert is named more than 16 times, a bound that some block reaches.
All inputs are finite; a program needn't handle non-finite values.
Results may differ from the reference program's by a relative error of at most 0.0095.
Values may be sent and summed in bfloat16 or wider, within the bound.
A program may use at most 128 MiB of HBM per device.

```python
import math
from functools import partial
import jax
import jax.numpy as jnp
import numpy as np
from jax import lax

D = 2048
DK = 64
CONTENT_WIDTH = 128
ATTENTION_LANES = 8
W_A = 1024
FF = 1024
GROUPS = 4
EXPERTS = 32
SPAN_STEPS = 512
T_DEV = 128
SEQS = 4
LEN = 1024
TOKENS = 4096
CAP = 16


def draw_log_forget_extra(key, part):
    first_key, second_key = jax.random.split(jax.random.fold_in(key, 17))
    places = jax.random.randint(first_key, (SEQS, ATTENTION_LANES, 4), 0, LEN)
    depth = jax.random.uniform(second_key, (SEQS, ATTENTION_LANES, 4), jnp.float32, 0.22, 0.69)
    positions = jnp.arange(LEN, dtype=jnp.int32)
    struck = places[:, :, :, None] == positions[None, None, None, :]
    return -jnp.sum(jnp.where(struck, depth[:, :, :, None], 0.0), axis=2).astype(jnp.float32)


def steps_of(own_key, extent, shards, smallest, largest):
    factor_of, own = 1.0, jax.random.fold_in(own_key, 6)
    for position, parts in shards:
        heights = jnp.exp(jax.random.uniform(jax.random.fold_in(own, position), (parts,), jnp.float32, smallest / len(shards), largest / len(shards)))
        factor_of = factor_of * jnp.repeat(heights, extent[position] // parts).reshape([-1 if axis == position else 1 for axis in range(len(extent))])
    return factor_of


def assign_block(key, own, number, rows, number_of, top, limit, skew):
    order = jax.random.permutation(key, number_of)
    heavy_load, ordinary = shares(number_of, rows * top, limit, skew, True), shares(number_of, rows * top, limit, skew, False)
    places = jnp.arange(number_of)

    def named(sizes, offset_by):
        used = int((sizes > 0).sum())
        fixed = max(1, used // 4)
        passed = fixed + (places - fixed + offset_by * (used - fixed)) % max(1, number_of - fixed)
        return jnp.zeros((number_of,), jnp.int32).at[order[jnp.where(places < fixed, places, passed)]].set(jnp.asarray(sizes, jnp.int32))

    sizes = jnp.where(number % 4 == 0, named(heavy_load, number // 4), named(ordinary, number - number // 4 - 1))
    mixed = jax.random.permutation(jax.random.fold_in(own, 3), number_of)
    donor, sink = mixed[0:number_of // 2 * 2:2], mixed[1:number_of // 2 * 2:2]
    slack = jnp.minimum(sizes[donor] - 1, limit - sizes[sink]) // 2
    slack = jnp.where((donor == order[0]) | (sink == order[0]) | (sizes[sink] == 0), 0, jnp.maximum(slack, 0))
    passed = jax.random.randint(jax.random.fold_in(own, 4), (number_of // 2,), 0, 1 << 20) % (slack + 1)
    sizes = sizes.at[donor].add(-passed).at[sink].add(passed)
    items = jnp.searchsorted(jnp.cumsum(sizes), jnp.arange(rows * top), side="right").astype(jnp.int32)
    listing = items.reshape(top, rows).T
    listing = listing[jax.random.permutation(jax.random.fold_in(own, 1), rows)]
    offset_by = jax.random.randint(jax.random.fold_in(own, 2), (rows, 1), 0, top)
    return jnp.take_along_axis(listing, (jnp.arange(top)[None, :] + offset_by) % top, axis=1)


def shares(count, total, bound, lean, full):
    loads = [(1 << 20) // math.isqrt(standing ** lean) + 1 for standing in range(1, count + 1)]
    largest = bound if full else min(bound, max(-(-total // count), total * loads[0] // sum(loads)))
    least = 1 if total - largest >= count - 1 else 0
    counts, spare = [largest] + [least] * (count - 1), total - largest - least * (count - 1)
    while spare > 0:
        movable = [i for i in range(1, count) if counts[i] < largest] or [i for i in range(1, count) if counts[i] < bound]
        pool, remaining = sum([loads[i] for i in movable]), spare
        for i in movable:
            extra = min(bound - counts[i], max(1, remaining * loads[i] // pool), spare)
            counts[i] = counts[i] + extra
            spare = spare - extra
    return np.array(counts)


def normal_values(own_key, extent, deviation, most, shards=(), held_as=jnp.bfloat16):
    factor_of = steps_of(own_key, extent, shards, -0.22, 0.18) if shards else 1.0
    result = jax.random.normal(own_key, extent, jnp.float32) * deviation * factor_of
    return jnp.minimum(jnp.maximum(result, -most), most).astype(held_as)


def setup_inputs(seed: int = 0) -> dict:
    arg_keys = jax.random.split(jax.random.key(seed), 19)
    residual_input = normal_values(arg_keys[0], (SEQS, LEN, D), 1.0, 6.0, ((0, 4), (1, 8)))
    queries = normal_values(arg_keys[1], (SEQS, LEN, ATTENTION_LANES * DK), 1.0, 6.0, ((0, 4), (1, 8)))
    keys = normal_values(arg_keys[2], (SEQS, LEN, ATTENTION_LANES * DK), 1.0, 6.0, ((0, 4), (1, 8)))
    values = normal_values(arg_keys[3], (SEQS, LEN, W_A), 1.0, 6.0, ((0, 4), (1, 8)))
    gate_logits = normal_values(arg_keys[4], (SEQS, LEN, 4 * ATTENTION_LANES), 1.0, 6.0, ((0, 4), (1, 8)))
    retention_offset = jnp.clip(3.0 + 9.0 * jax.random.uniform(arg_keys[5], (ATTENTION_LANES, 2), jnp.float32) ** steps_of(arg_keys[5], (ATTENTION_LANES, 2), ((0, 8),), -0.2, 0.2), 3.0, 12.0)
    log_forget_extra = draw_log_forget_extra(jax.random.fold_in(arg_keys[18], 71), 0)
    lane_amplifier = jnp.clip(1.0 + 0.18 * jax.random.normal(arg_keys[7], (W_A,), jnp.float32), 0.1, 1.9)
    output_gate_logits = normal_values(arg_keys[8], (SEQS, LEN, W_A), 1.0, 6.0, ((0, 4), (1, 8)))
    output_projection = normal_values(arg_keys[9], (W_A, D), W_A ** -0.5, 0.1875, ((1, 4),))
    cell_norm_gain = jnp.clip(1.0 + 0.18 * jax.random.normal(arg_keys[10], (D,), jnp.float32), 0.1, 1.9)
    expert_norm_gain = jnp.clip(1.0 + 0.18 * jax.random.normal(arg_keys[11], (D,), jnp.float32), 0.1, 1.9)
    expert_index_keys = jax.random.split(jax.random.fold_in(arg_keys[12], 1), SEQS * LEN // T_DEV)
    expert_index_turns = jax.random.permutation(jax.random.fold_in(arg_keys[12], 3), SEQS * LEN // T_DEV)
    expert_index = jax.vmap(lambda own, number: assign_block(jax.random.fold_in(arg_keys[12], 2), own, number, T_DEV, EXPERTS, 2, CAP, 2))(expert_index_keys, expert_index_turns).reshape((SEQS, LEN, 2))
    group_mixing_weight = jnp.clip(0.05 + 0.95 * jax.random.uniform(arg_keys[13], (SEQS, LEN, GROUPS), jnp.float32) ** steps_of(arg_keys[13], (SEQS, LEN, GROUPS), ((0, 4), (1, 8)), -0.2, 0.2), 0.05, 1.0)
    within_group_weight = jnp.clip(0.1 + 0.9 * jax.random.uniform(arg_keys[14], (SEQS, LEN, 2), jnp.float32) ** steps_of(arg_keys[14], (SEQS, LEN, 2), ((0, 4), (1, 8)), -0.2, 0.2), 0.1, 1.0)
    gate_weight = normal_values(arg_keys[15], (EXPERTS, D, FF), D ** -0.5, 0.125, ((0, 32),))
    up_weight = normal_values(arg_keys[16], (EXPERTS, D, FF), D ** -0.5, 0.125, ((0, 32),))
    down_weight = normal_values(arg_keys[17], (EXPERTS, FF, D), (FF // 16) ** -0.5, 0.75, ((0, 32),))
    return dict(residual_input=residual_input, queries=queries, keys=keys, values=values, gate_logits=gate_logits, retention_offset=retention_offset, log_forget_extra=log_forget_extra, lane_amplifier=lane_amplifier, output_gate_logits=output_gate_logits, output_projection=output_projection, cell_norm_gain=cell_norm_gain, expert_norm_gain=expert_norm_gain, expert_index=expert_index, group_mixing_weight=group_mixing_weight, within_group_weight=within_group_weight, gate_weight=gate_weight, up_weight=up_weight, down_weight=down_weight)


EPS = 1e-06
HIGH_PRECISION = lax.Precision.HIGHEST

def block_states(keys_f, values_f, in_gate, log_forget, span_steps):
    length, key_width = keys_f.shape
    blocks = length // span_steps
    blocked_keys = keys_f.reshape(blocks, span_steps, key_width)
    blocked_values = values_f.reshape(blocks, span_steps, values_f.shape[1])
    running = jnp.cumsum(log_forget.reshape(blocks, span_steps), axis=1)
    block_end = running[:, -1]
    weight_log = block_end[:, None] - running + in_gate.reshape(blocks, span_steps)
    local_top = lax.optimization_barrier(jnp.max(weight_log, axis=1))
    weight_table = jnp.exp(weight_log - local_top[:, None])
    local_memory = jnp.einsum('ryd,rya->rda', blocked_values * weight_table[:, :, None], blocked_keys, precision=HIGH_PRECISION)
    local_normalizer = jnp.einsum('nb,nby->ny', weight_table, blocked_keys, precision=HIGH_PRECISION)

    def advance(carried_state, inputs):
        memory, normal, stable = carried_state
        end_log, top_log, memory_new, normal_new = inputs
        raised = jnp.maximum(end_log + stable, top_log)
        keep_old = jnp.exp(end_log + stable - raised)
        keep_new = jnp.exp(top_log - raised)
        updated = (keep_old * memory + keep_new * memory_new, keep_old * normal + keep_new * normal_new, raised)
        return (updated, (memory, normal, stable))
    initial = (jnp.zeros((values_f.shape[1], key_width), jnp.float32), jnp.zeros((key_width,), jnp.float32), jnp.zeros((), jnp.float32))
    _, entries = lax.scan(advance, initial, (block_end, local_top, local_memory, local_normalizer))
    return entries

def direction_out(query_f, keys_f, values_f, in_gate, log_forget, span_steps):
    entry_memory, entry_normal, entry_top = block_states(keys_f, values_f, in_gate, log_forget, span_steps)
    length, key_width = keys_f.shape
    blocks = length // span_steps
    query_blocks = query_f.reshape(blocks, span_steps, key_width) * key_width ** (-0.5)
    blocked_keys = keys_f.reshape(blocks, span_steps, key_width)
    blocked_values = values_f.reshape(blocks, span_steps, values_f.shape[1])
    running = jnp.cumsum(log_forget.reshape(blocks, span_steps), axis=1)
    entry_log = running + entry_top[:, None]
    pair_log = running[:, :, None] - running[:, None, :] + in_gate.reshape(blocks, span_steps)[:, None, :]
    earlier = jnp.tril(jnp.ones((span_steps, span_steps), dtype=bool))
    pair_log = jnp.where(earlier[None], pair_log, -jnp.inf)
    top_log = jnp.maximum(entry_log, lax.optimization_barrier(jnp.max(pair_log, axis=2)))
    scores = jnp.einsum('ctk,csk->cts', query_blocks, blocked_keys, precision=HIGH_PRECISION) * jnp.exp(pair_log - top_log[:, :, None])
    carried = jnp.exp(entry_log - top_log)
    numerator = carried[:, :, None] * jnp.einsum('cvk,ctk->ctv', entry_memory, query_blocks, precision=HIGH_PRECISION)
    numerator = numerator + jnp.einsum('cts,csv->ctv', scores, blocked_values, precision=HIGH_PRECISION)
    denominator = carried * jnp.einsum('ck,ctk->ct', entry_normal, query_blocks, precision=HIGH_PRECISION) + lax.optimization_barrier(jnp.sum(scores, axis=2))
    output = numerator / jnp.maximum(jnp.abs(denominator), jnp.exp(-top_log))[:, :, None]
    return output.reshape(length, blocked_values.shape[2])

def lane_blend(lane_question, lane_addresses, lane_contents, lane_switches, lane_offset, lane_spread, lane_rescaling, span_steps):
    query_f = lane_question.astype(jnp.float32)
    keys_f = lane_addresses.astype(jnp.float32)
    values_f = lane_contents.astype(jnp.float32)
    retention_entries = lane_switches.astype(jnp.float32)
    onward_fading = jax.nn.log_sigmoid(retention_entries[:, 1] + lane_offset[0]) + lane_spread
    reverse_fading = jax.nn.log_sigmoid(retention_entries[:, 3] + lane_offset[1]) + lane_spread
    forward = direction_out(query_f, keys_f, values_f, retention_entries[:, 0], onward_fading, span_steps)
    backward = direction_out(query_f[::-1], keys_f[::-1], values_f[::-1], retention_entries[::-1, 2], reverse_fading[::-1], span_steps)[::-1]
    total = forward + backward
    normed = total * lax.rsqrt(lax.optimization_barrier(jnp.mean(total * total, axis=1, keepdims=True)) + EPS) * lane_rescaling
    return normed.astype(jnp.bfloat16)

def series_blender(series_question, series_addresses, series_contents, series_switches, series_spread, retention_offset, lane_amplifier):
    lane_question = series_question.reshape(LEN, ATTENTION_LANES, DK).transpose(1, 0, 2)
    lane_addresses = series_addresses.reshape(LEN, ATTENTION_LANES, DK).transpose(1, 0, 2)
    lane_contents = series_contents.reshape(LEN, ATTENTION_LANES, CONTENT_WIDTH).transpose(1, 0, 2)
    lane_switches = series_switches.reshape(LEN, ATTENTION_LANES, 4).transpose(1, 0, 2)
    return jax.vmap(partial(lane_blend, span_steps=SPAN_STEPS))(lane_question, lane_addresses, lane_contents, lane_switches, retention_offset, series_spread, lane_amplifier.reshape(ATTENTION_LANES, CONTENT_WIDTH))

def reference(residual_input, queries, keys, values, gate_logits, retention_offset, log_forget_extra, lane_amplifier, output_gate_logits, output_projection, cell_norm_gain, expert_norm_gain, expert_index, group_mixing_weight, within_group_weight, gate_weight, up_weight, down_weight):
    mixed_output = lax.map(lambda packed_rows: series_blender(packed_rows[0], packed_rows[1], packed_rows[2], packed_rows[3], packed_rows[4], retention_offset, lane_amplifier), (queries, keys, values, gate_logits, log_forget_extra))
    mixed_output = mixed_output.transpose(0, 2, 1, 3).reshape(TOKENS, W_A)
    gated = (mixed_output.astype(jnp.float32) * jax.nn.sigmoid(output_gate_logits.reshape(TOKENS, W_A).astype(jnp.float32))).astype(jnp.bfloat16)
    proj = jnp.dot(gated, output_projection, preferred_element_type=jnp.float32)
    stream_f = residual_input.reshape(TOKENS, D).astype(jnp.float32)
    stream = (stream_f + cell_norm_gain * proj * lax.rsqrt(lax.optimization_barrier(jnp.mean(proj * proj, axis=1, keepdims=True)) + EPS)).astype(jnp.bfloat16)
    stream_f = stream.astype(jnp.float32)
    moe_in = (expert_norm_gain * stream_f * lax.rsqrt(lax.optimization_barrier(jnp.mean(stream_f * stream_f, axis=1, keepdims=True)) + EPS)).astype(jnp.bfloat16)
    dev_blocks = TOKENS // T_DEV
    flat_ids = expert_index.reshape(TOKENS * 2)
    block_ids = flat_ids.reshape(dev_blocks, T_DEV * 2)
    onehot = (block_ids[:, :, None] == jnp.arange(EXPERTS, dtype=jnp.int32)[None, None, :]).astype(jnp.int32)
    slot_index = lax.optimization_barrier(jnp.sum((jnp.cumsum(onehot, axis=1) - onehot) * onehot, axis=2))
    column = (jnp.arange(dev_blocks, dtype=jnp.int32)[:, None] * CAP + slot_index).reshape(TOKENS * 2).astype(jnp.int32)
    token_of = (jnp.arange(TOKENS * 2, dtype=jnp.int32) // 2).astype(jnp.int32)
    group_of = expert_index.reshape(TOKENS, 2) // (EXPERTS // GROUPS)
    group_hit = (group_of[:, :, None] == jnp.arange(GROUPS, dtype=jnp.int32)[None, None, :]).astype(jnp.float32)
    chosen_group = lax.optimization_barrier(jnp.sum(group_mixing_weight.reshape(TOKENS, 1, GROUPS) * group_hit, axis=2))
    route = (chosen_group * within_group_weight.reshape(TOKENS, 2)).reshape(TOKENS * 2)
    table = jnp.full((EXPERTS, dev_blocks * CAP), TOKENS, jnp.int32).at[flat_ids, column].set(token_of)
    share = jnp.zeros((EXPERTS, dev_blocks * CAP), jnp.float32).at[flat_ids, column].set(route)
    padded = jnp.concatenate([moe_in, jnp.zeros((1, D), jnp.bfloat16)], axis=0)

    def expert_pass(total, inputs):
        rows_index, rows_share, gate_w, up_w, down_w = inputs
        picked = padded[rows_index]
        hidden = (jax.nn.silu(jnp.dot(picked, gate_w, preferred_element_type=jnp.float32)) * jnp.dot(picked, up_w, preferred_element_type=jnp.float32)).astype(jnp.bfloat16)
        produced = jnp.dot(hidden, down_w, preferred_element_type=jnp.float32).astype(jnp.bfloat16)
        return (total.at[rows_index].add(rows_share[:, None] * produced.astype(jnp.float32)), None)
    total, _ = lax.scan(expert_pass, jnp.zeros((TOKENS + 1, D), jnp.float32), (table, share, gate_weight, up_weight, down_weight))
    stream_out = (stream_f + total[:TOKENS]).astype(jnp.bfloat16)
    return stream_out.reshape(SEQS, LEN, D)
```

```python
from functools import partial

import jax
import jax.numpy as jnp
from jax import lax
from jax.experimental import pallas as pl
from jax.experimental.pallas import tpu as pltpu
from jax.sharding import PartitionSpec as P

EPS = 1e-06
MESH = pl.DeviceIdType.MESH
GATE_ROWS = 16


def log_sigmoid(x):
    return jnp.minimum(x, 0.0) - jnp.log1p(jnp.exp(-jnp.abs(x)))


def front_kernel(
    q_ref, k_ref, v_ref, g_ref, offset_ref, extra_ref, amp_ref, logits_ref, w_ref,
    res_ref, cell_gain_ref, expert_gain_ref,
    stream_ref, moe_ref,
    send, recv, gates_t, cols, mixed, mrecv, wfull, proj,
    send_sem, recv_sem, msend_sem, mrecv_sem, wx_send, wx_recv, wc_send, wc_recv, wl_sem,
    *, n, dpn,
):
    tok = q_ref.shape[1]
    dk = q_ref.shape[2] // n
    dv = v_ref.shape[2] // n
    length = n * tok
    wcol = w_ref.shape[1]
    me = lax.axis_index("sp")
    my_dp = lax.axis_index("dp")
    my_x, my_core = my_dp // 2, my_dp % 2
    chips = dpn // 2

    barrier = pltpu.get_barrier_semaphore()

    def greet(sp, dp):
        pl.semaphore_signal(
            barrier, inc=1, device_id={"sp": sp, "dp": dp}, device_id_type=MESH
        )

    for o in range(1, n):
        greet((me + o) % n, my_dp)
    for o in range(1, chips):
        greet(me, ((my_x + o) % chips) * 2 + my_core)
    greet(me, my_x * 2 + 1 - my_core)

    for h in range(n):
        send[h, 0:tok, 0:dk] = k_ref[0, :, h * dk : (h + 1) * dk]
        send[h, 0:tok, dk : 2 * dk] = q_ref[0, :, h * dk : (h + 1) * dk]
        send[h, 0:tok, 2 * dk : 2 * dk + dv] = v_ref[0, :, h * dv : (h + 1) * dv]
    g = g_ref[0].astype(jnp.float32)
    g = jnp.concatenate([g, jnp.zeros((tok, 128 - g.shape[1]), jnp.float32)], axis=1)
    gates_t[...] = g.T
    for h in range(n):
        send[h, tok : tok + GATE_ROWS, 0:tok] = gates_t[4 * h : 4 * h + GATE_ROWS, :].astype(
            jnp.bfloat16
        )
        send[h, tok : tok + GATE_ROWS, tok:] = jnp.zeros(
            (GATE_ROWS, send.shape[2] - tok), jnp.bfloat16
        )

    own_w = pltpu.make_async_copy(w_ref, wfull.at[my_dp], wl_sem)
    own_w.start()

    pl.semaphore_wait(barrier, n - 1 + chips - 1 + 1)

    def qkv_copy(o):
        return pltpu.make_async_remote_copy(
            src_ref=send.at[(me + o) % n],
            dst_ref=recv.at[me],
            send_sem=send_sem.at[o],
            recv_sem=recv_sem.at[o],
            device_id={"sp": (me + o) % n, "dp": my_dp},
            device_id_type=MESH,
        )

    def qkv_arrival(o):
        return pltpu.make_async_remote_copy(
            src_ref=send.at[(me + o) % n],
            dst_ref=recv.at[(me + n - o) % n],
            send_sem=send_sem.at[o],
            recv_sem=recv_sem.at[o],
            device_id={"sp": (me + o) % n, "dp": my_dp},
            device_id_type=MESH,
        )

    def wx_copy(o, slot):
        return pltpu.make_async_remote_copy(
            src_ref=w_ref,
            dst_ref=wfull.at[slot],
            send_sem=wx_send.at[o],
            recv_sem=wx_recv.at[o],
            device_id={"sp": me, "dp": ((my_x + o) % chips) * 2 + my_core},
            device_id_type=MESH,
        )

    def wc_copy(o, src, slot):
        return pltpu.make_async_remote_copy(
            src_ref=src,
            dst_ref=wfull.at[slot],
            send_sem=wc_send.at[o],
            recv_sem=wc_recv.at[o],
            device_id={"sp": me, "dp": my_x * 2 + 1 - my_core},
            device_id_type=MESH,
        )

    for o in range(1, n):
        qkv_copy(o).start()
    for o in range(1, chips):
        wx_copy(o, my_dp).start()
    wc_copy(0, w_ref, my_dp).start()
    recv[me] = send[me]
    for o in range(1, n):
        qkv_arrival(o).wait_recv()

    gates = jnp.concatenate(
        [recv[d, tok : tok + GATE_ROWS, 0:tok].astype(jnp.float32) for d in range(n)], axis=1
    )
    extra = extra_ref[0]
    f = log_sigmoid(gates[1:2] + offset_ref[0:1, 0:1]) + extra
    b = log_sigmoid(gates[3:4] + offset_ref[0:1, 1:2]) + extra
    f = jnp.broadcast_to(f, (8, length))
    b = jnp.broadcast_to(b, (8, length))
    lane = lax.broadcasted_iota(jnp.int32, (8, length), 1)
    step = 1
    while step < length:
        f = f + jnp.where(lane >= step, pltpu.roll(f, step, 1), 0.0)
        b = b + jnp.where(lane < length - step, pltpu.roll(b, length - step, 1), 0.0)
        step *= 2
    row_i = gates[0:1]
    row_f = row_i - f[0:1]
    row_b = gates[2:3] - b[0:1]
    sub = lax.broadcasted_iota(jnp.int32, (128, length), 0)
    stacked = jnp.where(sub == 0, f[0:1], jnp.where(sub == 1, b[0:1], row_i))
    cols[...] = stacked.T

    scale = dk ** (-0.5)
    amp = amp_ref[...]

    def mixed_copy(o, slot):
        return pltpu.make_async_remote_copy(
            src_ref=mixed.at[(me + o) % n],
            dst_ref=mrecv.at[slot],
            send_sem=msend_sem.at[o],
            recv_sem=mrecv_sem.at[o],
            device_id={"sp": (me + o) % n, "dp": my_dp},
            device_id_type=MESH,
        )

    def segment(j, _):
        d = (me + 1 + j) % n
        start = pl.multiple_of(d * tok, tok)
        kq = recv[d, 0:tok, 0 : 2 * dk]
        qs = kq[:, dk:].astype(jnp.float32) * scale
        ks = kq[:, :dk].astype(jnp.float32)
        diag = jnp.sum(qs * ks, axis=1, keepdims=True)
        qs = jnp.concatenate([qs, jnp.zeros_like(qs)], axis=1).astype(jnp.bfloat16)
        kall = recv[:, 0:tok, 0 : 2 * dk].reshape(length, 2 * dk)
        vall = recv[:, 0:tok, 2 * dk : 2 * dk + dv].reshape(length, dv)
        scores = lax.dot_general(
            qs, kall, (((1,), (1,)), ((), ())), preferred_element_type=jnp.float32
        )
        col = cols[pl.ds(start, tok), :]
        col_f, col_b, col_i = col[:, 0:1], col[:, 1:2], col[:, 2:3]
        t_pos = start + lax.broadcasted_iota(jnp.int32, (tok, length), 0)
        s_pos = lax.broadcasted_iota(jnp.int32, (tok, length), 1)
        before = s_pos < t_pos
        weight = scores * jnp.exp(jnp.where(before, col_f + row_f, col_b + row_b))
        diag = diag * jnp.exp(col_i)
        z_f = jnp.sum(jnp.where(before, weight, 0.0), axis=1, keepdims=True) + diag
        z_b = jnp.sum(jnp.where(before, 0.0, weight), axis=1, keepdims=True)
        inv_f = 1.0 / jnp.maximum(jnp.abs(z_f), 1.0)
        inv_b = 1.0 / jnp.maximum(jnp.abs(z_b), 1.0)
        probs = (weight * jnp.where(before, inv_f, inv_b)).astype(jnp.bfloat16)
        total = jnp.dot(probs, vall, preferred_element_type=jnp.float32)
        total = total + (diag * inv_f) * recv[d, 0:tok, 2 * dk : 2 * dk + dv].astype(jnp.float32)
        total = total * lax.rsqrt(jnp.mean(total * total, axis=1, keepdims=True) + EPS) * amp
        mixed[d] = total.astype(jnp.bfloat16)

        @pl.when(j >= 1)
        def _():
            mixed_copy(j, me).start()

        return 0

    lax.fori_loop(0, n, segment, 0)

    for o in range(1, chips):
        wx_copy(o, ((my_x + chips - o) % chips) * 2 + my_core).wait_recv()
        slot = ((my_x + chips - o) % chips) * 2 + my_core
        wc_copy(o, wfull.at[slot], slot).start()
    mrecv[me] = mixed[me]
    sig = jax.nn.sigmoid(logits_ref[0].astype(jnp.float32))
    for o in range(1, n):
        mixed_copy(o, (me + n - o) % n).wait_recv()
    gated = jnp.concatenate([mrecv[h].astype(jnp.float32) for h in range(n)], axis=1) * sig
    gated = gated.astype(jnp.bfloat16)
    own_w.wait()
    partner = 1 - my_core
    wc_copy(0, w_ref, my_x * 2 + partner).wait_recv()
    for o in range(1, chips):
        slot = ((my_x + chips - o) % chips) * 2 + partner
        wc_copy(o, wfull.at[slot], slot).wait_recv()
    for j in range(dpn):
        proj[:, j * wcol : (j + 1) * wcol] = jnp.dot(
            gated, wfull[j], preferred_element_type=jnp.float32
        )
    p = proj[...]
    stream = (
        res_ref[0].astype(jnp.float32)
        + cell_gain_ref[...] * p * lax.rsqrt(jnp.mean(p * p, axis=1, keepdims=True) + EPS)
    ).astype(jnp.bfloat16)
    stream_ref[...] = stream
    s = stream.astype(jnp.float32)
    moe_ref[...] = (
        expert_gain_ref[...] * s * lax.rsqrt(jnp.mean(s * s, axis=1, keepdims=True) + EPS)
    ).astype(jnp.bfloat16)

    for o in range(1, n):
        qkv_copy(o).wait_send()
        mixed_copy(o, me).wait_send()
    for o in range(1, chips):
        wx_copy(o, my_dp).wait_send()
        slot = ((my_x + chips - o) % chips) * 2 + my_core
        wc_copy(o, wfull.at[slot], slot).wait_send()
    wc_copy(0, w_ref, my_dp).wait_send()


def front(
    residual_input, queries, keys, values, gate_logits, retention_offset, log_forget_extra,
    lane_amplifier, output_gate_logits, output_projection, cell_norm_gain, expert_norm_gain,
):
    n, dpn = lax.axis_size("sp"), lax.axis_size("dp")
    tok, width = residual_input.shape[1:]
    dk, dv = queries.shape[2] // n, values.shape[2] // n
    length = n * tok
    dma = pltpu.SemaphoreType.DMA
    vmem = pl.BlockSpec(memory_space=pltpu.VMEM)
    return pl.pallas_call(
        partial(front_kernel, n=n, dpn=dpn),
        out_shape=(
            jax.ShapeDtypeStruct((tok, width), jnp.bfloat16),
            jax.ShapeDtypeStruct((tok, width), jnp.bfloat16),
        ),
        in_specs=[vmem] * 12,
        out_specs=(vmem, vmem),
        scratch_shapes=[
            pltpu.VMEM((n, tok + GATE_ROWS, 2 * dk + dv), jnp.bfloat16),
            pltpu.VMEM((n, tok + GATE_ROWS, 2 * dk + dv), jnp.bfloat16),
            pltpu.VMEM((128, tok), jnp.float32),
            pltpu.VMEM((length, 128), jnp.float32),
            pltpu.VMEM((n, tok, dv), jnp.bfloat16),
            pltpu.VMEM((n, tok, dv), jnp.bfloat16),
            pltpu.VMEM((dpn,) + output_projection.shape, jnp.bfloat16),
            pltpu.VMEM((tok, width), jnp.float32),
            dma((n,)), dma((n,)), dma((n,)), dma((n,)),
            dma((dpn // 2,)), dma((dpn // 2,)), dma((dpn // 2,)), dma((dpn // 2,)),
            dma(()),
        ],
        compiler_params=pltpu.CompilerParams(
            collective_id=0, has_side_effects=True, vmem_limit_bytes=48 * 1024 * 1024
        ),
    )(
        queries, keys, values, gate_logits, retention_offset, log_forget_extra,
        lane_amplifier.reshape(1, dv), output_gate_logits, output_projection,
        residual_input, cell_norm_gain.reshape(1, width), expert_norm_gain.reshape(1, width),
    )


def on_device(
    residual_input,
    queries,
    keys,
    values,
    gate_logits,
    retention_offset,
    log_forget_extra,
    lane_amplifier,
    output_gate_logits,
    output_projection,
    cell_norm_gain,
    expert_norm_gain,
    expert_index,
    group_mixing_weight,
    within_group_weight,
    gate_weight,
    up_weight,
    down_weight,
):
    tok_rows, width = residual_input.shape[1:]
    stream, moe_in = front(
        residual_input, queries, keys, values, gate_logits, retention_offset, log_forget_extra,
        lane_amplifier, output_gate_logits, output_projection, cell_norm_gain, expert_norm_gain,
    )
    stream_f = stream.astype(jnp.float32)
    seq_devices = lax.axis_size("sp")
    seq_groups = lax.axis_size("dp")
    experts = seq_devices * seq_groups
    capacity = 4 * tok_rows // experts
    flat_ids = expert_index.reshape(tok_rows * 2)
    onehot = (flat_ids[:, None] == jnp.arange(experts, dtype=jnp.int32)[None, :]).astype(jnp.int32)
    slot_index = jnp.sum((jnp.cumsum(onehot, axis=0) - onehot) * onehot, axis=1)
    target = flat_ids * capacity + slot_index
    slot_table = (
        target[:, None] == jnp.arange(experts * capacity, dtype=jnp.int32)[None, :]
    ).astype(jnp.bfloat16)
    token_table = jnp.sum(slot_table.reshape(tok_rows, 2, experts * capacity), axis=1)
    outgoing = lax.dot_general(
        token_table, moe_in, (((0,), (0,)), ((), ())), preferred_element_type=jnp.float32
    ).astype(jnp.bfloat16)
    incoming = lax.all_to_all(outgoing, ("sp", "dp"), split_axis=0, concat_axis=0, tiled=True)
    hidden = (
        jax.nn.silu(jnp.dot(incoming, gate_weight[0], preferred_element_type=jnp.float32))
        * jnp.dot(incoming, up_weight[0], preferred_element_type=jnp.float32)
    ).astype(jnp.bfloat16)
    produced = jnp.dot(hidden, down_weight[0], preferred_element_type=jnp.float32).astype(
        jnp.bfloat16
    )
    returned = lax.all_to_all(produced, ("sp", "dp"), split_axis=0, concat_axis=0, tiled=True)
    group_count = group_mixing_weight.shape[2]
    group_of = expert_index.reshape(tok_rows, 2) // (experts // group_count)
    group_hit = (
        group_of[:, :, None] == jnp.arange(group_count, dtype=jnp.int32)[None, None, :]
    ).astype(jnp.float32)
    chosen_group = jnp.sum(
        group_mixing_weight.reshape(tok_rows, 1, group_count) * group_hit, axis=2
    )
    route = chosen_group * within_group_weight.reshape(tok_rows, 2)
    picked = jnp.dot(slot_table, returned, preferred_element_type=jnp.float32).reshape(
        tok_rows, 2, width
    )
    mixture = jnp.sum(picked * route[:, :, None], axis=1)
    return (stream_f + mixture).astype(jnp.bfloat16).reshape(1, tok_rows, width)


def solution(mesh):
    in_specs = (
        P("dp", "sp", None),
        P("dp", "sp", None),
        P("dp", "sp", None),
        P("dp", "sp", None),
        P("dp", "sp", None),
        P("sp", None),
        P("dp", "sp", None),
        P("sp"),
        P("dp", "sp", None),
        P(None, "dp"),
        P(),
        P(),
        P("dp", "sp", None),
        P("dp", "sp", None),
        P("dp", "sp", None),
        P(("sp", "dp"), None, None),
        P(("sp", "dp"), None, None),
        P(("sp", "dp"), None, None),
    )
    out_specs = P("dp", "sp", None)
    return jax.shard_map(
        on_device, mesh=mesh, in_specs=in_specs, out_specs=out_specs, check_vma=False
    )
```

```python
from functools import partial

import jax
import jax.numpy as jnp
from jax import lax
from jax.experimental import pallas as pl
from jax.experimental.pallas import tpu as pltpu
from jax.sharding import PartitionSpec as P

EPS = 1e-06
MESH = pl.DeviceIdType.MESH
GATE_ROWS = 16
CHUNKS = 4
FF_TILE = 256


def log_sigmoid(x):
    return jnp.minimum(x, 0.0) - jnp.log1p(jnp.exp(-jnp.abs(x)))


def layer_kernel(*refs, n, dpn, inputs):
    hbm, (out_ref,), rest = refs[:inputs], refs[inputs : inputs + 1], refs[inputs + 1 :]
    local, rest = rest[:inputs], rest[inputs:]
    (
        q_ref, k_ref, v_ref, g_ref, offset_ref, extra_ref, amp_ref, logits_ref, w_ref,
        res_ref, cell_gain_ref, expert_gain_ref, index_ref, group_ref, within_ref,
        gate_ref, up_ref, down_ref,
    ) = local
    (
        send, recv, gates_t, cols, mixed, mrecv, wfull, proj,
        moe, table_t, table_0, table_1, outgoing, incoming, xs, hs, produced, returned,
        in_sem, send_sem, recv_sem, msend_sem, mrecv_sem, wx_send, wx_recv, wc_send, wc_recv,
        wl_sem, out_send, out_recv, back_send, back_recv,
    ) = rest
    loads = [pltpu.make_async_copy(hbm[i], local[i], in_sem.at[i]) for i in range(inputs)]
    for load in loads:
        load.start()
    tok = q_ref.shape[1]
    dk = q_ref.shape[2] // n
    dv = v_ref.shape[2] // n
    length = n * tok
    wcol = w_ref.shape[1]
    me = lax.axis_index("sp")
    my_dp = lax.axis_index("dp")
    my_x, my_core = my_dp // 2, my_dp % 2
    chips = dpn // 2

    barrier = pltpu.get_barrier_semaphore()

    devices = n * dpn
    mine = me * dpn + my_dp
    cap = 4 * tok // devices
    per = devices // CHUNKS
    my_chunk, my_place = mine // per, mine % per

    def greet(o, _):
        other = (mine + o) % devices
        pl.semaphore_signal(
            barrier,
            inc=1,
            device_id={"sp": other // dpn, "dp": other % dpn},
            device_id_type=MESH,
        )
        return 0

    lax.fori_loop(1, devices, greet, 0)
    for load in loads[:4]:
        load.wait()

    for h in range(n):
        send[h, 0:tok, 0:dk] = k_ref[0, :, h * dk : (h + 1) * dk]
        send[h, 0:tok, dk : 2 * dk] = q_ref[0, :, h * dk : (h + 1) * dk]
        send[h, 0:tok, 2 * dk : 2 * dk + dv] = v_ref[0, :, h * dv : (h + 1) * dv]
    g = g_ref[0].astype(jnp.float32)
    g = jnp.concatenate([g, jnp.zeros((tok, 128 - g.shape[1]), jnp.float32)], axis=1)
    gates_t[...] = g.T
    for h in range(n):
        send[h, tok : tok + GATE_ROWS, 0:tok] = gates_t[4 * h : 4 * h + GATE_ROWS, :].astype(
            jnp.bfloat16
        )
        send[h, tok : tok + GATE_ROWS, tok:] = jnp.zeros(
            (GATE_ROWS, send.shape[2] - tok), jnp.bfloat16
        )

    pl.semaphore_wait(barrier, devices - 1)

    def qkv_copy(o):
        return pltpu.make_async_remote_copy(
            src_ref=send.at[(me + o) % n],
            dst_ref=recv.at[me],
            send_sem=send_sem.at[o],
            recv_sem=recv_sem.at[o],
            device_id={"sp": (me + o) % n, "dp": my_dp},
            device_id_type=MESH,
        )

    def qkv_arrival(o):
        return pltpu.make_async_remote_copy(
            src_ref=send.at[(me + o) % n],
            dst_ref=recv.at[(me + n - o) % n],
            send_sem=send_sem.at[o],
            recv_sem=recv_sem.at[o],
            device_id={"sp": (me + o) % n, "dp": my_dp},
            device_id_type=MESH,
        )

    def wx_copy(o, slot):
        return pltpu.make_async_remote_copy(
            src_ref=w_ref,
            dst_ref=wfull.at[slot],
            send_sem=wx_send.at[o],
            recv_sem=wx_recv.at[o],
            device_id={"sp": me, "dp": ((my_x + o) % chips) * 2 + my_core},
            device_id_type=MESH,
        )

    def wc_copy(o, src, slot):
        return pltpu.make_async_remote_copy(
            src_ref=src,
            dst_ref=wfull.at[slot],
            send_sem=wc_send.at[o],
            recv_sem=wc_recv.at[o],
            device_id={"sp": me, "dp": my_x * 2 + 1 - my_core},
            device_id_type=MESH,
        )

    for o in range(1, n):
        qkv_copy(o).start()
    loads[8].wait()
    for o in range(1, chips):
        wx_copy(o, my_dp).start()
    wc_copy(0, w_ref, my_dp).start()
    own_w = pltpu.make_async_copy(w_ref, wfull.at[my_dp], wl_sem)
    own_w.start()
    recv[me] = send[me]
    for i in (4, 5, 6, 7, 9, 10, 11, 12, 13, 14):
        loads[i].wait()

    rows_in = per * cap
    ids = index_ref[0].astype(jnp.float32)
    e_0, e_1 = ids[:, 0:1], ids[:, 1:2]
    wide = -(-devices // 128) * 128
    lane_e = lax.broadcasted_iota(jnp.int32, (tok, wide), 1).astype(jnp.float32)
    hit_0 = jnp.where(lane_e == e_0, 1.0, 0.0)
    hit_1 = jnp.where(lane_e == e_1, 1.0, 0.0)
    tri = jnp.where(
        lax.broadcasted_iota(jnp.int32, (tok, tok), 1)
        < lax.broadcasted_iota(jnp.int32, (tok, tok), 0),
        1.0,
        0.0,
    ).astype(jnp.bfloat16)
    rank_0 = jnp.dot(tri, hit_0.astype(jnp.bfloat16), preferred_element_type=jnp.float32)
    rank_1 = jnp.dot(tri, hit_1.astype(jnp.bfloat16), preferred_element_type=jnp.float32)
    rank_1 = rank_1 + jnp.sum(hit_0, axis=0, keepdims=True)
    place_0 = e_0 * cap + jnp.sum(hit_0 * rank_0, axis=1, keepdims=True)
    place_1 = e_1 * cap + jnp.sum(hit_1 * rank_1, axis=1, keepdims=True)
    lane_t = lax.broadcasted_iota(jnp.int32, (tok, tok), 1)
    turned = jnp.where(lane_t == 0, place_0, place_1).T
    row_0, row_1 = turned[0:1], turned[1:2]
    sub_r = lax.broadcasted_iota(jnp.int32, (rows_in, tok), 0).astype(jnp.float32)
    lane_r = lax.broadcasted_iota(jnp.int32, (tok, rows_in), 1).astype(jnp.float32)
    for c in range(CHUNKS):
        at = sub_r + c * rows_in
        table_t[c] = (jnp.where(at == row_0, 1.0, 0.0) + jnp.where(at == row_1, 1.0, 0.0)).astype(
            jnp.bfloat16
        )
        at = lane_r + c * rows_in
        table_0[c] = jnp.where(at == place_0, 1.0, 0.0).astype(jnp.bfloat16)
        table_1[c] = jnp.where(at == place_1, 1.0, 0.0).astype(jnp.bfloat16)
    groups = group_ref.shape[2]
    span = devices // groups
    route_0 = jnp.zeros((tok, 1), jnp.float32)
    route_1 = jnp.zeros((tok, 1), jnp.float32)
    for c in range(groups):
        weight_c = group_ref[0, :, c : c + 1]
        route_0 += jnp.where((e_0 >= c * span) & (e_0 < (c + 1) * span), weight_c, 0.0)
        route_1 += jnp.where((e_1 >= c * span) & (e_1 < (c + 1) * span), weight_c, 0.0)
    route_0 = route_0 * within_ref[0, :, 0:1]
    route_1 = route_1 * within_ref[0, :, 1:2]

    for o in range(1, n):
        qkv_arrival(o).wait_recv()

    gates = jnp.concatenate(
        [recv[d, tok : tok + GATE_ROWS, 0:tok].astype(jnp.float32) for d in range(n)], axis=1
    )
    extra = extra_ref[0]
    f = log_sigmoid(gates[1:2] + offset_ref[0:1, 0:1]) + extra
    b = log_sigmoid(gates[3:4] + offset_ref[0:1, 1:2]) + extra
    f = jnp.broadcast_to(f, (8, length))
    b = jnp.broadcast_to(b, (8, length))
    lane = lax.broadcasted_iota(jnp.int32, (8, length), 1)
    step = 1
    while step < length:
        f = f + jnp.where(lane >= step, pltpu.roll(f, step, 1), 0.0)
        b = b + jnp.where(lane < length - step, pltpu.roll(b, length - step, 1), 0.0)
        step *= 2
    row_i = gates[0:1]
    row_f = row_i - f[0:1]
    row_b = gates[2:3] - b[0:1]
    sub = lax.broadcasted_iota(jnp.int32, (128, length), 0)
    stacked = jnp.where(sub == 0, f[0:1], jnp.where(sub == 1, b[0:1], row_i))
    cols[...] = stacked.T

    scale = dk ** (-0.5)
    amp = amp_ref[...]

    def mixed_copy(o, slot):
        return pltpu.make_async_remote_copy(
            src_ref=mixed.at[(me + o) % n],
            dst_ref=mrecv.at[slot],
            send_sem=msend_sem.at[o],
            recv_sem=mrecv_sem.at[o],
            device_id={"sp": (me + o) % n, "dp": my_dp},
            device_id_type=MESH,
        )

    def segment(j, _):
        d = (me + 1 + j) % n
        start = pl.multiple_of(d * tok, tok)
        kq = recv[d, 0:tok, 0 : 2 * dk]
        qs = kq[:, dk:].astype(jnp.float32) * scale
        ks = kq[:, :dk].astype(jnp.float32)
        diag = jnp.sum(qs * ks, axis=1, keepdims=True)
        qs = jnp.concatenate([qs, jnp.zeros_like(qs)], axis=1).astype(jnp.bfloat16)
        kall = recv[:, 0:tok, 0 : 2 * dk].reshape(length, 2 * dk)
        vall = recv[:, 0:tok, 2 * dk : 2 * dk + dv].reshape(length, dv)
        scores = lax.dot_general(
            qs, kall, (((1,), (1,)), ((), ())), preferred_element_type=jnp.float32
        )
        col = cols[pl.ds(start, tok), :]
        col_f, col_b, col_i = col[:, 0:1], col[:, 1:2], col[:, 2:3]
        t_pos = start + lax.broadcasted_iota(jnp.int32, (tok, length), 0)
        s_pos = lax.broadcasted_iota(jnp.int32, (tok, length), 1)
        before = s_pos < t_pos
        weight = scores * jnp.exp(jnp.where(before, col_f + row_f, col_b + row_b))
        diag = diag * jnp.exp(col_i)
        z_f = jnp.sum(jnp.where(before, weight, 0.0), axis=1, keepdims=True) + diag
        z_b = jnp.sum(jnp.where(before, 0.0, weight), axis=1, keepdims=True)
        inv_f = 1.0 / jnp.maximum(jnp.abs(z_f), 1.0)
        inv_b = 1.0 / jnp.maximum(jnp.abs(z_b), 1.0)
        probs = (weight * jnp.where(before, inv_f, inv_b)).astype(jnp.bfloat16)
        total = jnp.dot(probs, vall, preferred_element_type=jnp.float32)
        total = total + (diag * inv_f) * recv[d, 0:tok, 2 * dk : 2 * dk + dv].astype(jnp.float32)
        total = total * lax.rsqrt(jnp.mean(total * total, axis=1, keepdims=True) + EPS) * amp
        mixed[d] = total.astype(jnp.bfloat16)

        @pl.when(j >= 1)
        def _():
            mixed_copy(j, me).start()

        return 0

    lax.fori_loop(0, n, segment, 0)

    for o in range(1, chips):
        wx_copy(o, ((my_x + chips - o) % chips) * 2 + my_core).wait_recv()
        slot = ((my_x + chips - o) % chips) * 2 + my_core
        wc_copy(o, wfull.at[slot], slot).start()
    mrecv[me] = mixed[me]
    sig = jax.nn.sigmoid(logits_ref[0].astype(jnp.float32))
    for o in range(1, n):
        mixed_copy(o, (me + n - o) % n).wait_recv()
    gated = jnp.concatenate([mrecv[h].astype(jnp.float32) for h in range(n)], axis=1) * sig
    gated = gated.astype(jnp.bfloat16)
    own_w.wait()
    partner = 1 - my_core
    wc_copy(0, w_ref, my_x * 2 + partner).wait_recv()
    for o in range(1, chips):
        slot = ((my_x + chips - o) % chips) * 2 + partner
        wc_copy(o, wfull.at[slot], slot).wait_recv()
    for j in range(dpn):
        proj[:, j * wcol : (j + 1) * wcol] = jnp.dot(
            gated, wfull[j], preferred_element_type=jnp.float32
        )
    p = proj[...]
    stream = (
        res_ref[0].astype(jnp.float32)
        + cell_gain_ref[...] * p * lax.rsqrt(jnp.mean(p * p, axis=1, keepdims=True) + EPS)
    ).astype(jnp.bfloat16)
    s = stream.astype(jnp.float32)
    proj[...] = s
    moe[...] = (
        expert_gain_ref[...] * s * lax.rsqrt(jnp.mean(s * s, axis=1, keepdims=True) + EPS)
    ).astype(jnp.bfloat16)

    width = moe.shape[1]

    def copy_of(src, dst, sems, tag, dev, slot_src, slot_dst):
        return pltpu.make_async_remote_copy(
            src_ref=src.at[slot_src],
            dst_ref=dst.at[slot_dst],
            send_sem=sems[0].at[tag],
            recv_sem=sems[1].at[tag],
            device_id={"sp": dev // dpn, "dp": dev % dpn},
            device_id_type=MESH,
        )

    def ahead(z, i):
        return (my_chunk + z) % CHUNKS * per + (my_place + i) % per

    def behind(z, i):
        return (my_chunk + CHUNKS - z) % CHUNKS * per + (my_place + per - i) % per

    out_sems, back_sems = (out_send, out_recv), (back_send, back_recv)

    def each(z, act):
        def one(i, _):
            @pl.when(z * per + i > 0)
            def _():
                act(i)

            return 0

        lax.fori_loop(0, per, one, 0)

    def dispatch(z, _):
        c = (my_chunk + z) % CHUNKS
        block = jnp.dot(table_t[c], moe[...], preferred_element_type=jnp.float32)
        outgoing[pl.ds(c * per, per)] = block.astype(jnp.bfloat16).reshape(per, cap, width)

        def start(i):
            dev = ahead(z, i)
            copy_of(outgoing, incoming, out_sems, z * per + i, dev, dev, mine).start()

        each(z, start)
        return 0

    lax.fori_loop(0, CHUNKS, dispatch, 0)
    incoming[mine] = outgoing[mine]
    for i in (15, 16, 17):
        loads[i].wait()
    ff = hs.shape[1]

    def expert(z, _):
        c = (my_chunk + CHUNKS - z) % CHUNKS

        def arrive(i):
            dev = behind(z, i)
            copy_of(outgoing, incoming, out_sems, z * per + i, dev, dev, dev).wait_recv()

        each(z, arrive)
        xs[...] = incoming[pl.ds(c * per, per)].reshape(rows_in, width)

        def up_tile(t, _):
            at = pl.ds(pl.multiple_of(t * FF_TILE, FF_TILE), FF_TILE)
            x = xs[...]
            a = jnp.dot(x, gate_ref[0, :, at], preferred_element_type=jnp.float32)
            u = jnp.dot(x, up_ref[0, :, at], preferred_element_type=jnp.float32)
            hs[:, at] = (jax.nn.silu(a) * u).astype(jnp.bfloat16)
            return 0

        lax.fori_loop(0, ff // FF_TILE, up_tile, 0)

        def down_tile(t, _):
            at = pl.ds(pl.multiple_of(t * FF_TILE, FF_TILE), FF_TILE)
            y = jnp.dot(hs[...], down_ref[0, :, at], preferred_element_type=jnp.float32)
            produced[pl.ds(c * per, per), :, at] = y.astype(jnp.bfloat16).reshape(
                per, cap, FF_TILE
            )
            return 0

        lax.fori_loop(0, width // FF_TILE, down_tile, 0)

        def start(i):
            dev = behind(z, i)
            copy_of(produced, returned, back_sems, z * per + i, dev, dev, mine).start()

        each(z, start)
        return 0

    lax.fori_loop(0, CHUNKS, expert, 0)
    returned[mine] = produced[mine]

    def combine(z, _):
        c = (my_chunk + z) % CHUNKS

        def arrive(i):
            dev = ahead(z, i)
            copy_of(produced, returned, back_sems, z * per + i, dev, dev, dev).wait_recv()

        each(z, arrive)
        block = returned[pl.ds(c * per, per)].reshape(rows_in, width)
        proj[...] += route_0 * jnp.dot(
            table_0[c], block, preferred_element_type=jnp.float32
        ) + route_1 * jnp.dot(table_1[c], block, preferred_element_type=jnp.float32)
        return 0

    lax.fori_loop(0, CHUNKS, combine, 0)
    out_ref[0] = proj[...].astype(jnp.bfloat16)

    def drain(z, _):
        def left(i):
            dev = ahead(z, i)
            copy_of(outgoing, incoming, out_sems, z * per + i, dev, dev, mine).wait_send()
            dev = behind(z, i)
            copy_of(produced, returned, back_sems, z * per + i, dev, dev, mine).wait_send()

        each(z, left)
        return 0

    lax.fori_loop(0, CHUNKS, drain, 0)
    for o in range(1, n):
        qkv_copy(o).wait_send()
        mixed_copy(o, me).wait_send()
    for o in range(1, chips):
        wx_copy(o, my_dp).wait_send()
        slot = ((my_x + chips - o) % chips) * 2 + my_core
        wc_copy(o, wfull.at[slot], slot).wait_send()
    wc_copy(0, w_ref, my_dp).wait_send()


def on_device(
    residual_input,
    queries,
    keys,
    values,
    gate_logits,
    retention_offset,
    log_forget_extra,
    lane_amplifier,
    output_gate_logits,
    output_projection,
    cell_norm_gain,
    expert_norm_gain,
    expert_index,
    group_mixing_weight,
    within_group_weight,
    gate_weight,
    up_weight,
    down_weight,
):
    n, dpn = lax.axis_size("sp"), lax.axis_size("dp")
    tok, width = residual_input.shape[1:]
    dk, dv = queries.shape[2] // n, values.shape[2] // n
    length, devices, ff = n * tok, n * dpn, gate_weight.shape[2]
    cap, per = 4 * tok // devices, devices // CHUNKS
    rows_in = per * cap
    operands = (
        queries, keys, values, gate_logits, retention_offset, log_forget_extra,
        lane_amplifier.reshape(1, dv), output_gate_logits, output_projection,
        residual_input, cell_norm_gain.reshape(1, width), expert_norm_gain.reshape(1, width),
        expert_index, group_mixing_weight, within_group_weight,
        gate_weight, up_weight, down_weight,
    )
    dma = pltpu.SemaphoreType.DMA
    bf16, f32 = jnp.bfloat16, jnp.float32
    hbm = pl.BlockSpec(memory_space=pltpu.HBM)
    return pl.pallas_call(
        partial(layer_kernel, n=n, dpn=dpn, inputs=len(operands)),
        out_shape=jax.ShapeDtypeStruct((1, tok, width), bf16),
        in_specs=[hbm] * len(operands),
        out_specs=pl.BlockSpec(memory_space=pltpu.VMEM),
        scratch_shapes=[pltpu.VMEM(x.shape, x.dtype) for x in operands]
        + [
            pltpu.VMEM((n, tok + GATE_ROWS, 2 * dk + dv), bf16),
            pltpu.VMEM((n, tok + GATE_ROWS, 2 * dk + dv), bf16),
            pltpu.VMEM((128, tok), f32),
            pltpu.VMEM((length, 128), f32),
            pltpu.VMEM((n, tok, dv), bf16),
            pltpu.VMEM((n, tok, dv), bf16),
            pltpu.VMEM((dpn,) + output_projection.shape, bf16),
            pltpu.VMEM((tok, width), f32),
            pltpu.VMEM((tok, width), bf16),
            pltpu.VMEM((CHUNKS, rows_in, tok), bf16),
            pltpu.VMEM((CHUNKS, tok, rows_in), bf16),
            pltpu.VMEM((CHUNKS, tok, rows_in), bf16),
            pltpu.VMEM((devices, cap, width), bf16),
            pltpu.VMEM((devices, cap, width), bf16),
            pltpu.VMEM((rows_in, width), bf16),
            pltpu.VMEM((rows_in, ff), bf16),
            pltpu.VMEM((devices, cap, width), bf16),
            pltpu.VMEM((devices, cap, width), bf16),
            dma((len(operands),)),
            dma((n,)), dma((n,)), dma((n,)), dma((n,)),
            dma((dpn // 2,)), dma((dpn // 2,)), dma((dpn // 2,)), dma((dpn // 2,)),
            dma(()),
            dma((devices,)), dma((devices,)), dma((devices,)), dma((devices,)),
        ],
        compiler_params=pltpu.CompilerParams(
            collective_id=0, has_side_effects=True, vmem_limit_bytes=60 * 1024 * 1024
        ),
    )(*operands)


def solution(mesh):
    in_specs = (
        P("dp", "sp", None),
        P("dp", "sp", None),
        P("dp", "sp", None),
        P("dp", "sp", None),
        P("dp", "sp", None),
        P("sp", None),
        P("dp", "sp", None),
        P("sp"),
        P("dp", "sp", None),
        P(None, "dp"),
        P(),
        P(),
        P("dp", "sp", None),
        P("dp", "sp", None),
        P("dp", "sp", None),
        P(("sp", "dp"), None, None),
        P(("sp", "dp"), None, None),
        P(("sp", "dp"), None, None),
    )
    out_specs = P("dp", "sp", None)
    return jax.shard_map(
        on_device, mesh=mesh, in_specs=in_specs, out_specs=out_specs, check_vma=False
    )
```

```python
from functools import partial

import jax
import jax.numpy as jnp
from jax import lax
from jax.experimental import pallas as pl
from jax.experimental.pallas import tpu as pltpu
from jax.sharding import PartitionSpec as P

EPS = 1e-06
MESH = pl.DeviceIdType.MESH
GATE_ROWS = 16
CHUNKS = 4
FF_TILE = 256
PIECES = 4


def log_sigmoid(x):
    return jnp.minimum(x, 0.0) - jnp.log1p(jnp.exp(-jnp.abs(x)))


def layer_kernel(*refs, n, dpn, inputs):
    hbm, (out_ref,), rest = refs[:inputs], refs[inputs : inputs + 1], refs[inputs + 1 :]
    local, rest = rest[:inputs], rest[inputs:]
    (
        q_ref, k_ref, v_ref, g_ref, offset_ref, extra_ref, amp_ref, logits_ref, w_ref,
        res_ref, cell_gain_ref, expert_gain_ref, index_ref, group_ref, within_ref,
        gate_ref, up_ref, down_ref,
    ) = local
    (
        send, recv, gates_t, cols, mixed, mrecv, wfull, proj,
        moe, table_t, table_0, table_1, outgoing, incoming, xs, hs, produced, returned,
        in_sem, send_sem, recv_sem, msend_sem, mrecv_sem, wx_send, wx_recv, wc_send, wc_recv,
        wl_sem, out_send, out_recv, back_send, back_recv,
    ) = rest
    loads = [pltpu.make_async_copy(hbm[i], local[i], in_sem.at[i]) for i in range(inputs)]
    for load in loads:
        load.start()
    tok = q_ref.shape[1]
    dk = q_ref.shape[2] // n
    dv = v_ref.shape[2] // n
    length = n * tok
    wcol = w_ref.shape[1]
    me = lax.axis_index("sp")
    my_dp = lax.axis_index("dp")
    my_x, my_core = my_dp // 2, my_dp % 2
    chips = dpn // 2

    barrier = pltpu.get_barrier_semaphore()

    devices = n * dpn
    mine = me * dpn + my_dp
    cap = 4 * tok // devices
    per = devices // CHUNKS
    my_chunk, my_place = mine // per, mine % per

    def greet(o, _):
        other = (mine + o) % devices
        pl.semaphore_signal(
            barrier,
            inc=1,
            device_id={"sp": other // dpn, "dp": other % dpn},
            device_id_type=MESH,
        )
        return 0

    lax.fori_loop(1, devices, greet, 0)
    for load in loads[:4]:
        load.wait()

    for h in range(n):
        send[h, 0:tok, 0:dk] = k_ref[0, :, h * dk : (h + 1) * dk]
        send[h, 0:tok, dk : 2 * dk] = q_ref[0, :, h * dk : (h + 1) * dk]
        send[h, 0:tok, 2 * dk : 2 * dk + dv] = v_ref[0, :, h * dv : (h + 1) * dv]
    g = g_ref[0].astype(jnp.float32)
    g = jnp.concatenate([g, jnp.zeros((tok, 128 - g.shape[1]), jnp.float32)], axis=1)
    gates_t[...] = g.T
    for h in range(n):
        send[h, tok : tok + GATE_ROWS, 0:tok] = gates_t[4 * h : 4 * h + GATE_ROWS, :].astype(
            jnp.bfloat16
        )
        send[h, tok : tok + GATE_ROWS, tok:] = jnp.zeros(
            (GATE_ROWS, send.shape[2] - tok), jnp.bfloat16
        )

    pl.semaphore_wait(barrier, devices - 1)

    def qkv_copy(o):
        return pltpu.make_async_remote_copy(
            src_ref=send.at[(me + o) % n],
            dst_ref=recv.at[me],
            send_sem=send_sem.at[o],
            recv_sem=recv_sem.at[o],
            device_id={"sp": (me + o) % n, "dp": my_dp},
            device_id_type=MESH,
        )

    def qkv_arrival(o):
        return pltpu.make_async_remote_copy(
            src_ref=send.at[(me + o) % n],
            dst_ref=recv.at[(me + n - o) % n],
            send_sem=send_sem.at[o],
            recv_sem=recv_sem.at[o],
            device_id={"sp": (me + o) % n, "dp": my_dp},
            device_id_type=MESH,
        )

    piece = w_ref.shape[0] // PIECES

    def wx_copy(o, p, slot):
        return pltpu.make_async_remote_copy(
            src_ref=w_ref.at[pl.ds(p * piece, piece)],
            dst_ref=wfull.at[slot, pl.ds(p * piece, piece)],
            send_sem=wx_send.at[o, p],
            recv_sem=wx_recv.at[o, p],
            device_id={"sp": me, "dp": ((my_x + o) % chips) * 2 + my_core},
            device_id_type=MESH,
        )

    def wc_copy(o, p, src, slot):
        return pltpu.make_async_remote_copy(
            src_ref=src.at[pl.ds(p * piece, piece)],
            dst_ref=wfull.at[slot, pl.ds(p * piece, piece)],
            send_sem=wc_send.at[o, p],
            recv_sem=wc_recv.at[o, p],
            device_id={"sp": me, "dp": my_x * 2 + 1 - my_core},
            device_id_type=MESH,
        )

    def from_chip(o):
        return ((my_x + chips - o) % chips) * 2 + my_core

    def pass_on(p):
        for o in range(1, chips):
            slot = from_chip(o)
            wx_copy(o, p, slot).wait_recv()
            wc_copy(o, p, wfull.at[slot], slot).start()

    for o in range(1, n):
        qkv_copy(o).start()
    loads[8].wait()
    for p in range(PIECES):
        for o in range(1, chips):
            wx_copy(o, p, my_dp).start()
        wc_copy(0, p, w_ref, my_dp).start()
    own_w = pltpu.make_async_copy(w_ref, wfull.at[my_dp], wl_sem)
    own_w.start()
    recv[me] = send[me]
    for i in (4, 5, 6, 7, 9, 10, 11, 12, 13, 14):
        loads[i].wait()

    rows_in = per * cap
    ids = index_ref[0].astype(jnp.float32)
    e_0, e_1 = ids[:, 0:1], ids[:, 1:2]
    wide = -(-devices // 128) * 128
    lane_e = lax.broadcasted_iota(jnp.int32, (tok, wide), 1).astype(jnp.float32)
    hit_0 = jnp.where(lane_e == e_0, 1.0, 0.0)
    hit_1 = jnp.where(lane_e == e_1, 1.0, 0.0)
    tri = jnp.where(
        lax.broadcasted_iota(jnp.int32, (tok, tok), 1)
        < lax.broadcasted_iota(jnp.int32, (tok, tok), 0),
        1.0,
        0.0,
    ).astype(jnp.bfloat16)
    rank_0 = jnp.dot(tri, hit_0.astype(jnp.bfloat16), preferred_element_type=jnp.float32)
    rank_1 = jnp.dot(tri, hit_1.astype(jnp.bfloat16), preferred_element_type=jnp.float32)
    rank_1 = rank_1 + jnp.sum(hit_0, axis=0, keepdims=True)
    place_0 = e_0 * cap + jnp.sum(hit_0 * rank_0, axis=1, keepdims=True)
    place_1 = e_1 * cap + jnp.sum(hit_1 * rank_1, axis=1, keepdims=True)
    lane_t = lax.broadcasted_iota(jnp.int32, (tok, tok), 1)
    turned = jnp.where(lane_t == 0, place_0, place_1).T
    row_0, row_1 = turned[0:1], turned[1:2]
    sub_r = lax.broadcasted_iota(jnp.int32, (rows_in, tok), 0).astype(jnp.float32)
    lane_r = lax.broadcasted_iota(jnp.int32, (tok, rows_in), 1).astype(jnp.float32)
    for c in range(CHUNKS):
        at = sub_r + c * rows_in
        table_t[c] = (jnp.where(at == row_0, 1.0, 0.0) + jnp.where(at == row_1, 1.0, 0.0)).astype(
            jnp.bfloat16
        )
        at = lane_r + c * rows_in
        table_0[c] = jnp.where(at == place_0, 1.0, 0.0).astype(jnp.bfloat16)
        table_1[c] = jnp.where(at == place_1, 1.0, 0.0).astype(jnp.bfloat16)
    groups = group_ref.shape[2]
    span = devices // groups
    route_0 = jnp.zeros((tok, 1), jnp.float32)
    route_1 = jnp.zeros((tok, 1), jnp.float32)
    for c in range(groups):
        weight_c = group_ref[0, :, c : c + 1]
        route_0 += jnp.where((e_0 >= c * span) & (e_0 < (c + 1) * span), weight_c, 0.0)
        route_1 += jnp.where((e_1 >= c * span) & (e_1 < (c + 1) * span), weight_c, 0.0)
    route_0 = route_0 * within_ref[0, :, 0:1]
    route_1 = route_1 * within_ref[0, :, 1:2]

    for o in range(1, n):
        qkv_arrival(o).wait_recv()

    gates = jnp.concatenate(
        [recv[d, tok : tok + GATE_ROWS, 0:tok].astype(jnp.float32) for d in range(n)], axis=1
    )
    extra = extra_ref[0]
    f = log_sigmoid(gates[1:2] + offset_ref[0:1, 0:1]) + extra
    b = log_sigmoid(gates[3:4] + offset_ref[0:1, 1:2]) + extra
    f = jnp.broadcast_to(f, (8, length))
    b = jnp.broadcast_to(b, (8, length))
    lane = lax.broadcasted_iota(jnp.int32, (8, length), 1)
    step = 1
    while step < length:
        f = f + jnp.where(lane >= step, pltpu.roll(f, step, 1), 0.0)
        b = b + jnp.where(lane < length - step, pltpu.roll(b, length - step, 1), 0.0)
        step *= 2
    row_i = gates[0:1]
    row_f = row_i - f[0:1]
    row_b = gates[2:3] - b[0:1]
    sub = lax.broadcasted_iota(jnp.int32, (128, length), 0)
    stacked = jnp.where(sub == 0, f[0:1], jnp.where(sub == 1, b[0:1], row_i))
    cols[...] = stacked.T

    scale = dk ** (-0.5)
    amp = amp_ref[...]

    def mixed_copy(o, slot):
        return pltpu.make_async_remote_copy(
            src_ref=mixed.at[(me + o) % n],
            dst_ref=mrecv.at[slot],
            send_sem=msend_sem.at[o],
            recv_sem=mrecv_sem.at[o],
            device_id={"sp": (me + o) % n, "dp": my_dp},
            device_id_type=MESH,
        )

    def segment(j, _):
        d = (me + 1 + j) % n
        start = pl.multiple_of(d * tok, tok)
        kq = recv[d, 0:tok, 0 : 2 * dk]
        qs = kq[:, dk:].astype(jnp.float32) * scale
        ks = kq[:, :dk].astype(jnp.float32)
        diag = jnp.sum(qs * ks, axis=1, keepdims=True)
        qs = jnp.concatenate([qs, jnp.zeros_like(qs)], axis=1).astype(jnp.bfloat16)
        kall = recv[:, 0:tok, 0 : 2 * dk].reshape(length, 2 * dk)
        vall = recv[:, 0:tok, 2 * dk : 2 * dk + dv].reshape(length, dv)
        scores = lax.dot_general(
            qs, kall, (((1,), (1,)), ((), ())), preferred_element_type=jnp.float32
        )
        col = cols[pl.ds(start, tok), :]
        col_f, col_b, col_i = col[:, 0:1], col[:, 1:2], col[:, 2:3]
        t_pos = start + lax.broadcasted_iota(jnp.int32, (tok, length), 0)
        s_pos = lax.broadcasted_iota(jnp.int32, (tok, length), 1)
        before = s_pos < t_pos
        weight = scores * jnp.exp(jnp.where(before, col_f + row_f, col_b + row_b))
        diag = diag * jnp.exp(col_i)
        z_f = jnp.sum(jnp.where(before, weight, 0.0), axis=1, keepdims=True) + diag
        z_b = jnp.sum(jnp.where(before, 0.0, weight), axis=1, keepdims=True)
        inv_f = 1.0 / jnp.maximum(jnp.abs(z_f), 1.0)
        inv_b = 1.0 / jnp.maximum(jnp.abs(z_b), 1.0)
        probs = (weight * jnp.where(before, inv_f, inv_b)).astype(jnp.bfloat16)
        total = jnp.dot(probs, vall, preferred_element_type=jnp.float32)
        total = total + (diag * inv_f) * recv[d, 0:tok, 2 * dk : 2 * dk + dv].astype(jnp.float32)
        total = total * lax.rsqrt(jnp.mean(total * total, axis=1, keepdims=True) + EPS) * amp
        mixed[d] = total.astype(jnp.bfloat16)

        @pl.when(j >= 1)
        def _():
            mixed_copy(j, me).start()

        @pl.when(j == n // 2)
        def _():
            pass_on(PIECES - 2)

        return 0

    for p in range(PIECES - 2):
        pass_on(p)
    lax.fori_loop(0, n, segment, 0)
    pass_on(PIECES - 1)
    mrecv[me] = mixed[me]
    sig = jax.nn.sigmoid(logits_ref[0].astype(jnp.float32))
    for o in range(1, n):
        mixed_copy(o, (me + n - o) % n).wait_recv()
    gated = jnp.concatenate([mrecv[h].astype(jnp.float32) for h in range(n)], axis=1) * sig
    gated = gated.astype(jnp.bfloat16)
    own_w.wait()
    partner = 1 - my_core
    for p in range(PIECES):
        wc_copy(0, p, w_ref, my_x * 2 + partner).wait_recv()
        for o in range(1, chips):
            slot = ((my_x + chips - o) % chips) * 2 + partner
            wc_copy(o, p, wfull.at[slot], slot).wait_recv()
    for j in range(dpn):
        proj[:, j * wcol : (j + 1) * wcol] = jnp.dot(
            gated, wfull[j], preferred_element_type=jnp.float32
        )
    p = proj[...]
    stream = (
        res_ref[0].astype(jnp.float32)
        + cell_gain_ref[...] * p * lax.rsqrt(jnp.mean(p * p, axis=1, keepdims=True) + EPS)
    ).astype(jnp.bfloat16)
    s = stream.astype(jnp.float32)
    proj[...] = s
    moe[...] = (
        expert_gain_ref[...] * s * lax.rsqrt(jnp.mean(s * s, axis=1, keepdims=True) + EPS)
    ).astype(jnp.bfloat16)

    width = moe.shape[1]

    def copy_of(src, dst, sems, tag, dev, slot_src, slot_dst):
        return pltpu.make_async_remote_copy(
            src_ref=src.at[slot_src],
            dst_ref=dst.at[slot_dst],
            send_sem=sems[0].at[tag],
            recv_sem=sems[1].at[tag],
            device_id={"sp": dev // dpn, "dp": dev % dpn},
            device_id_type=MESH,
        )

    def ahead(z, i):
        return (my_chunk + z) % CHUNKS * per + (my_place + i) % per

    def behind(z, i):
        return (my_chunk + CHUNKS - z) % CHUNKS * per + (my_place + per - i) % per

    out_sems, back_sems = (out_send, out_recv), (back_send, back_recv)

    def each(z, act):
        def one(i, _):
            @pl.when(z * per + i > 0)
            def _():
                act(i)

            return 0

        lax.fori_loop(0, per, one, 0)

    def dispatch(turn, _):
        z = (turn + 1) % CHUNKS
        c = (my_chunk + z) % CHUNKS
        block = jnp.dot(table_t[c], moe[...], preferred_element_type=jnp.float32)
        outgoing[pl.ds(c * per, per)] = block.astype(jnp.bfloat16).reshape(per, cap, width)

        def start(i):
            dev = ahead(z, i)
            copy_of(outgoing, incoming, out_sems, z * per + i, dev, dev, mine).start()

        each(z, start)
        return 0

    lax.fori_loop(0, CHUNKS, dispatch, 0)
    incoming[mine] = outgoing[mine]
    for i in (15, 16, 17):
        loads[i].wait()
    ff = hs.shape[1]

    def expert(turn, _):
        z = (turn + 1) % CHUNKS
        c = (my_chunk + CHUNKS - z) % CHUNKS

        def arrive(i):
            dev = behind(z, i)
            copy_of(outgoing, incoming, out_sems, z * per + i, dev, dev, dev).wait_recv()

        each(z, arrive)
        xs[...] = incoming[pl.ds(c * per, per)].reshape(rows_in, width)

        def up_tile(t, _):
            at = pl.ds(pl.multiple_of(t * FF_TILE, FF_TILE), FF_TILE)
            x = xs[...]
            a = jnp.dot(x, gate_ref[0, :, at], preferred_element_type=jnp.float32)
            u = jnp.dot(x, up_ref[0, :, at], preferred_element_type=jnp.float32)
            hs[:, at] = (jax.nn.silu(a) * u).astype(jnp.bfloat16)
            return 0

        lax.fori_loop(0, ff // FF_TILE, up_tile, 0)

        def down_tile(t, _):
            at = pl.ds(pl.multiple_of(t * FF_TILE, FF_TILE), FF_TILE)
            y = jnp.dot(hs[...], down_ref[0, :, at], preferred_element_type=jnp.float32)
            produced[pl.ds(c * per, per), :, at] = y.astype(jnp.bfloat16).reshape(
                per, cap, FF_TILE
            )
            return 0

        lax.fori_loop(0, width // FF_TILE, down_tile, 0)

        def start(i):
            dev = behind(z, i)
            copy_of(produced, returned, back_sems, z * per + i, dev, dev, mine).start()

        each(z, start)
        return 0

    lax.fori_loop(0, CHUNKS, expert, 0)
    returned[mine] = produced[mine]

    def combine(turn, _):
        z = (turn + 1) % CHUNKS
        c = (my_chunk + z) % CHUNKS

        def arrive(i):
            dev = ahead(z, i)
            copy_of(produced, returned, back_sems, z * per + i, dev, dev, dev).wait_recv()

        each(z, arrive)
        block = returned[pl.ds(c * per, per)].reshape(rows_in, width)
        proj[...] += route_0 * jnp.dot(
            table_0[c], block, preferred_element_type=jnp.float32
        ) + route_1 * jnp.dot(table_1[c], block, preferred_element_type=jnp.float32)
        return 0

    lax.fori_loop(0, CHUNKS, combine, 0)
    out_ref[0] = proj[...].astype(jnp.bfloat16)

    def drain(z, _):
        def left(i):
            dev = ahead(z, i)
            copy_of(outgoing, incoming, out_sems, z * per + i, dev, dev, mine).wait_send()
            dev = behind(z, i)
            copy_of(produced, returned, back_sems, z * per + i, dev, dev, mine).wait_send()

        each(z, left)
        return 0

    lax.fori_loop(0, CHUNKS, drain, 0)
    for o in range(1, n):
        qkv_copy(o).wait_send()
        mixed_copy(o, me).wait_send()
    for p in range(PIECES):
        for o in range(1, chips):
            wx_copy(o, p, my_dp).wait_send()
            slot = from_chip(o)
            wc_copy(o, p, wfull.at[slot], slot).wait_send()
        wc_copy(0, p, w_ref, my_dp).wait_send()


def on_device(
    residual_input,
    queries,
    keys,
    values,
    gate_logits,
    retention_offset,
    log_forget_extra,
    lane_amplifier,
    output_gate_logits,
    output_projection,
    cell_norm_gain,
    expert_norm_gain,
    expert_index,
    group_mixing_weight,
    within_group_weight,
    gate_weight,
    up_weight,
    down_weight,
):
    n, dpn = lax.axis_size("sp"), lax.axis_size("dp")
    tok, width = residual_input.shape[1:]
    dk, dv = queries.shape[2] // n, values.shape[2] // n
    length, devices, ff = n * tok, n * dpn, gate_weight.shape[2]
    cap, per = 4 * tok // devices, devices // CHUNKS
    rows_in = per * cap
    operands = (
        queries, keys, values, gate_logits, retention_offset, log_forget_extra,
        lane_amplifier.reshape(1, dv), output_gate_logits, output_projection,
        residual_input, cell_norm_gain.reshape(1, width), expert_norm_gain.reshape(1, width),
        expert_index, group_mixing_weight, within_group_weight,
        gate_weight, up_weight, down_weight,
    )
    dma = pltpu.SemaphoreType.DMA
    bf16, f32 = jnp.bfloat16, jnp.float32
    hbm = pl.BlockSpec(memory_space=pltpu.HBM)
    return pl.pallas_call(
        partial(layer_kernel, n=n, dpn=dpn, inputs=len(operands)),
        out_shape=jax.ShapeDtypeStruct((1, tok, width), bf16),
        in_specs=[hbm] * len(operands),
        out_specs=pl.BlockSpec(memory_space=pltpu.VMEM),
        scratch_shapes=[pltpu.VMEM(x.shape, x.dtype) for x in operands]
        + [
            pltpu.VMEM((n, tok + GATE_ROWS, 2 * dk + dv), bf16),
            pltpu.VMEM((n, tok + GATE_ROWS, 2 * dk + dv), bf16),
            pltpu.VMEM((128, tok), f32),
            pltpu.VMEM((length, 128), f32),
            pltpu.VMEM((n, tok, dv), bf16),
            pltpu.VMEM((n, tok, dv), bf16),
            pltpu.VMEM((dpn,) + output_projection.shape, bf16),
            pltpu.VMEM((tok, width), f32),
            pltpu.VMEM((tok, width), bf16),
            pltpu.VMEM((CHUNKS, rows_in, tok), bf16),
            pltpu.VMEM((CHUNKS, tok, rows_in), bf16),
            pltpu.VMEM((CHUNKS, tok, rows_in), bf16),
            pltpu.VMEM((devices, cap, width), bf16),
            pltpu.VMEM((devices, cap, width), bf16),
            pltpu.VMEM((rows_in, width), bf16),
            pltpu.VMEM((rows_in, ff), bf16),
            pltpu.VMEM((devices, cap, width), bf16),
            pltpu.VMEM((devices, cap, width), bf16),
            dma((len(operands),)),
            dma((n,)), dma((n,)), dma((n,)), dma((n,)),
            dma((dpn // 2, PIECES)), dma((dpn // 2, PIECES)),
            dma((dpn // 2, PIECES)), dma((dpn // 2, PIECES)),
            dma(()),
            dma((devices,)), dma((devices,)), dma((devices,)), dma((devices,)),
        ],
        compiler_params=pltpu.CompilerParams(
            collective_id=0, has_side_effects=True, vmem_limit_bytes=60 * 1024 * 1024
        ),
    )(*operands)


def solution(mesh):
    in_specs = (
        P("dp", "sp", None),
        P("dp", "sp", None),
        P("dp", "sp", None),
        P("dp", "sp", None),
        P("dp", "sp", None),
        P("sp", None),
        P("dp", "sp", None),
        P("sp"),
        P("dp", "sp", None),
        P(None, "dp"),
        P(),
        P(),
        P("dp", "sp", None),
        P("dp", "sp", None),
        P("dp", "sp", None),
        P(("sp", "dp"), None, None),
        P(("sp", "dp"), None, None),
        P(("sp", "dp"), None, None),
    )
    out_specs = P("dp", "sp", None)
    return jax.shard_map(
        on_device, mesh=mesh, in_specs=in_specs, out_specs=out_specs, check_vma=False
    )
```
